256 devices in a mesh: ep: 128 (over z, y, x), tp: 2 (over core).
Axes of the slice: x: 4, y: 4, z: 8, core: 2. Of those that a mesh axis runs over, the one named last changes fastest.
Arguments:
- tokens: bfloat16 [4096, 1024], P('ep'), may hold values from -6 to 6
- norm_gain: float32 [1024], replicated, may hold values from 0.1 to 1.9
- routing: int32 [4096, 4], P('ep'), may hold values from 0 to 127, all different within a row; in each aligned block of 32 rows (0 to 31, 32 to 63, ...) at most 16 rows name the same one
- route_logits: float32 [4096, 4], P('ep'), may hold values from -6 to 6
- w_gate: bfloat16 [128, 1024, 1024], P('ep', None, 'tp'), may hold values from -0.1875 to 0.1875
- w_up: bfloat16 [128, 1024, 1024], P('ep', None, 'tp'), may hold values from -0.1875 to 0.1875
- w_down: bfloat16 [128, 1024, 1024], P('ep', None, 'tp'), may hold values from -0.1875 to 0.1875
Outputs:
- mixed: bfloat16 [4096, 1024], P('ep', 'tp')
The draws below stay inside these ranges and needn't reach their ends.
Inputs may be any that keep to these rules, and one draw needn't show every extreme that they name: `routing`: each row names 4 different experts; among the 32 tokens of one index of ep (aligned blocks of rows) no expert is named by more than 16 rows, and some block has an expert named by exactly 16.
All inputs are finite; a program needn't handle non-finite values.
Results may differ from the reference program's by a relative error of at most 0.0085.
Values may be sent and summed in bfloat16 or wider, within the bound.
No kernel may reach another device: no remote copies, remote signals or barrier semaphores. Data moves between devices by JAX's collectives and lax.ppermute only.
A program may use at most 64 MiB of HBM per device.

```python
import math
import jax
import jax.numpy as jnp
import numpy as np
from jax import lax

D = 1024
FF = 1024
TOPK = 4
TOK_DEV = 32
TOKENS = 4096
EXPERTS = 128
CAP = 16


def block_levels(stream_key, dims, shards, smallest, largest):
    def one(axis_at, parts):
        steps = jax.random.uniform(jax.random.fold_in(jax.random.fold_in(stream_key, 6), axis_at), (parts,), jnp.float32, smallest / len(shards), largest / len(shards))
        return jnp.repeat(jnp.exp(steps), dims[axis_at] // parts).reshape((-1,) + (1,) * (len(dims) - axis_at - 1))

    level = one(*shards[0])
    for cut in shards[1:]:
        level = level * one(*cut)
    return level


def routed_block(stream_key, own, number, rows, count, top, reach, skew):
    ranking = jax.random.permutation(stream_key, count)
    packed, ordinary = portions_of(count, rows * top, reach, skew, True), portions_of(count, rows * top, reach, skew, False)
    places = jnp.arange(count)

    def named(tallies, rotation):
        used = int((tallies > 0).sum())
        fixed = max(1, used // 4)
        passed = fixed + (places - fixed + rotation * (used - fixed)) % max(1, count - fixed)
        return jnp.zeros((count,), jnp.int32).at[ranking[jnp.where(places < fixed, places, passed)]].set(jnp.asarray(tallies, jnp.int32))

    tallies = jnp.where(number % 4 == 0, named(packed, number // 4), named(ordinary, number - number // 4 - 1))
    mixed = jax.random.permutation(jax.random.fold_in(own, 3), count)
    donor, taker = mixed[0:count // 2 * 2:2], mixed[1:count // 2 * 2:2]
    slack = jnp.minimum(tallies[donor] - 1, reach - tallies[taker]) // 2
    slack = jnp.where((donor == ranking[0]) | (taker == ranking[0]) | (tallies[taker] == 0), 0, jnp.maximum(slack, 0))
    passed = jax.random.randint(jax.random.fold_in(own, 4), (count // 2,), 0, 1 << 20) % (slack + 1)
    tallies = tallies.at[donor].add(-passed).at[taker].add(passed)
    members = jnp.searchsorted(jnp.cumsum(tallies), jnp.arange(rows * top), side="right").astype(jnp.int32)
    listing = members.reshape(top, rows).T
    listing = listing[jax.random.permutation(jax.random.fold_in(own, 1), rows)]
    rotation = jax.random.randint(jax.random.fold_in(own, 2), (rows, 1), 0, top)
    return jnp.take_along_axis(listing, (jnp.arange(top)[None, :] + rotation) % top, axis=1)


def portions_of(amount, total, bound, lean, full):
    portions = [(1 << 20) // math.isqrt(rank ** lean) + 1 for rank in range(1, amount + 1)]
    largest = bound if full else min(bound, max(-(-total // amount), total * portions[0] // sum(portions)))
    least = 1 if total - largest >= amount - 1 else 0
    given, surplus = [largest] + [least] * (amount - 1), total - largest - least * (amount - 1)
    while surplus > 0:
        candidates = [i for i in range(1, amount) if given[i] < largest] or [i for i in range(1, amount) if given[i] < bound]
        pool, remaining = sum([portions[i] for i in candidates]), surplus
        for i in candidates:
            more = min(bound - given[i], max(1, remaining * portions[i] // pool), surplus)
            given[i] = given[i] + more
            surplus = surplus - more
    return np.array(given)


def bell_draw(key, shape, spread, most, split=(), held_as=jnp.bfloat16):
    array = jax.random.normal(key, shape, jnp.float32) * spread
    if len(split) > 0:
        array = block_levels(key, shape, split, -0.22, 0.18) * array
    return jnp.clip(array, min=-most, max=most).astype(held_as)


def setup_inputs(seed: int = 0) -> dict:
    key_list = jax.random.split(jax.random.key(seed), 8)
    tokens = bell_draw(key_list[0], (TOKENS, D), 1.0, 6.0, ((0, 128),))
    norm_gain = jnp.clip(1.0 + 0.18 * jax.random.normal(key_list[1], (D,), jnp.float32), 0.1, 1.9)
    routing_keys = jax.random.split(jax.random.fold_in(key_list[2], 1), TOKENS // TOK_DEV)
    routing_turns = jax.random.permutation(jax.random.fold_in(key_list[2], 3), TOKENS // TOK_DEV)
    routing = jax.vmap(lambda own, number: routed_block(jax.random.fold_in(key_list[2], 2), own, number, TOK_DEV, EXPERTS, TOPK, CAP, 2))(routing_keys, routing_turns).reshape((TOKENS, TOPK))
    route_logits = bell_draw(key_list[3], (TOKENS, TOPK), 1.5, 6.0, ((0, 128),), jnp.float32)
    w_gate = bell_draw(key_list[4], (EXPERTS, D, FF), D ** -0.5, 0.1875, ((0, 128), (2, 2)))
    w_up = bell_draw(key_list[5], (EXPERTS, D, FF), D ** -0.5, 0.1875, ((0, 128), (2, 2)))
    w_down = bell_draw(key_list[6], (EXPERTS, FF, D), FF ** -0.5, 0.1875, ((0, 128), (2, 2)))
    return dict(tokens=tokens, norm_gain=norm_gain, routing=routing, route_logits=route_logits, w_gate=w_gate, w_up=w_up, w_down=w_down)


eps = 1e-5


def clamped(gate_part, up_part):
    limited = jnp.minimum(gate_part, 7.0)
    linear = jnp.clip(up_part, -7.0, 7.0)
    return limited * jax.nn.sigmoid(1.702 * limited) * (linear + 1.0)


def reference(tokens, norm_gain, routing, route_logits, w_gate, w_up, w_down):
    as_float = tokens.astype(jnp.float32)
    scaled = as_float * lax.rsqrt(jnp.mean(as_float * as_float, axis=-1, keepdims=True) + eps)
    normed = (scaled * norm_gain).astype(jnp.bfloat16)
    probs = jax.nn.softmax(route_logits, axis=-1)
    count_tok = routing.shape[0]
    topk = routing.shape[1]
    assigns = count_tok * topk
    block_rows = 32
    flat_e = routing.reshape(-1).astype(jnp.int32)
    flat_tok = (jnp.arange(assigns, dtype=jnp.int32) // topk).astype(jnp.int32)
    flat_w = probs.reshape(-1)
    order = jnp.argsort(flat_e, stable=True).astype(jnp.int32)
    sorted_e = flat_e[order]
    counts = jnp.bincount(flat_e, length=EXPERTS).astype(jnp.int32)
    starts = (jnp.cumsum(counts) - counts).astype(jnp.int32)
    padded = ((counts + block_rows - 1) // block_rows * block_rows).astype(jnp.int32)
    pends = jnp.cumsum(padded).astype(jnp.int32)
    pstarts = (pends - padded).astype(jnp.int32)
    dest = (pstarts[sorted_e] + jnp.arange(assigns, dtype=jnp.int32) - starts[sorted_e]).astype(jnp.int32)
    n_blocks = -(-assigns // block_rows) + EXPERTS
    n_rows = n_blocks * block_rows
    row_tok = jnp.full((n_rows,), count_tok, dtype=jnp.int32).at[dest].set(flat_tok[order])
    row_w = jnp.zeros((n_rows,), jnp.float32).at[dest].set(flat_w[order])
    block_e = jnp.minimum(
        jnp.searchsorted(pends, jnp.arange(n_blocks, dtype=jnp.int32) * block_rows, side="right").astype(jnp.int32),
        EXPERTS - 1).astype(jnp.int32)
    x_pad = jnp.concatenate([normed, jnp.zeros((1, normed.shape[1]), jnp.bfloat16)], axis=0)
    blocks_in = x_pad[row_tok].reshape(n_blocks, block_rows, normed.shape[1])

    def expert_block(pair):
        rows, expert = pair
        gate_part = jnp.dot(rows, w_gate[expert], preferred_element_type=jnp.float32)
        up_part = jnp.dot(rows, w_up[expert], preferred_element_type=jnp.float32)
        hidden = clamped(gate_part, up_part).astype(jnp.bfloat16)
        return jnp.dot(hidden, w_down[expert], preferred_element_type=jnp.float32).astype(jnp.bfloat16)

    outs_rows = lax.map(expert_block, (blocks_in, block_e)).reshape(n_rows, normed.shape[1])
    summed = jax.ops.segment_sum(outs_rows.astype(jnp.float32) * row_w[:, None], row_tok, num_segments=count_tok + 1)
    return summed[:count_tok].astype(jnp.bfloat16)
```

```python
import jax
import jax.numpy as jnp
from jax import lax
from jax.sharding import PartitionSpec as P

eps = 1e-05


def clamped(gate_part, up_part):
    limited = jnp.minimum(gate_part, 7.0)
    linear = jnp.clip(up_part, -7.0, 7.0)
    return limited * jax.nn.sigmoid(1.702 * limited) * (linear + 1.0)


def shards(tokens, norm_gain, routing, route_logits, w_gate, w_up, w_down):
    core = lax.axis_index("tp")
    expert = lax.axis_index("ep")
    half = tokens.shape[0] // 2
    width = tokens.shape[1]
    mine = lax.dynamic_slice_in_dim(tokens, core * half, half, 0)
    routes = lax.dynamic_slice_in_dim(routing, core * half, half, 0)
    logits = lax.dynamic_slice_in_dim(route_logits, core * half, half, 0)

    gate_full = lax.all_gather(w_gate[0], "tp", axis=1, tiled=True)
    up_full = lax.all_gather(w_up[0], "tp", axis=1, tiled=True)
    down_full = lax.all_gather(w_down[0], "tp", axis=1, tiled=True)

    as_float = mine.astype(jnp.float32)
    scaled = as_float * lax.rsqrt(jnp.mean(as_float * as_float, axis=-1, keepdims=True) + eps)
    normed = (scaled * norm_gain).astype(jnp.bfloat16)
    probs = jax.nn.softmax(logits, axis=-1)

    rows = lax.all_gather(normed, "ep", axis=0, tiled=True)
    all_routes = lax.all_gather(routes, "ep", axis=0, tiled=True)
    all_probs = lax.all_gather(probs, "ep", axis=0, tiled=True)
    share = jnp.sum(jnp.where(all_routes == expert, all_probs, 0.0), axis=1, keepdims=True)

    gate_part = jnp.dot(rows, gate_full, preferred_element_type=jnp.float32)
    up_part = jnp.dot(rows, up_full, preferred_element_type=jnp.float32)
    hidden = clamped(gate_part, up_part).astype(jnp.bfloat16)
    out = jnp.dot(hidden, down_full, preferred_element_type=jnp.float32)
    out = (out * share).astype(jnp.bfloat16)
    mixed = lax.psum_scatter(out, "ep", scatter_dimension=0, tiled=True)
    return lax.all_to_all(mixed, "tp", split_axis=1, concat_axis=0, tiled=True)


def solution(mesh):
    return jax.shard_map(
        shards,
        mesh=mesh,
        in_specs=(
            P("ep", None),
            P(),
            P("ep", None),
            P("ep", None),
            P("ep", None, "tp"),
            P("ep", None, "tp"),
            P("ep", None, "tp"),
        ),
        out_specs=P("ep", "tp"),
        check_vma=False,
    )
```

```python
import functools

import jax
import jax.numpy as jnp
from jax import lax
from jax.experimental import pallas as pl
from jax.experimental.pallas import tpu as pltpu
from jax.sharding import Mesh, PartitionSpec as P

CAP = 16
NZ, NY, NX = 8, 4, 4
PLANE = NY * NX
TOPK = 4
TOK = 32
BLOCKS = NZ // 2
SLOTS = BLOCKS * CAP
HELD = BLOCKS * TOK
ROWS = PLANE * SLOTS
META = 8
EPS = 1e-05
MIB = 1 << 20

BF16, F32, I32 = jnp.bfloat16, jnp.float32, jnp.int32
VMEM = pl.BlockSpec(memory_space=pltpu.VMEM)
SMEM = pl.BlockSpec(memory_space=pltpu.SMEM)


def dot(a, b, dims=((1,), (0,))):
    return lax.dot_general(a, b, (dims, ((), ())), preferred_element_type=F32)


def split_two(x):
    high = x.astype(BF16)
    return high, (x - high.astype(F32)).astype(BF16)


def norm_kernel(tokens, gain, routes, logits, out):
    x = tokens[...].astype(F32)
    scale = lax.rsqrt(jnp.mean(x * x, axis=-1, keepdims=True) + EPS)
    out[:TOK, :] = (x * scale * gain[...]).astype(BF16)
    e = jnp.exp(logits[...] - jnp.max(logits[...], axis=0, keepdims=True))
    probs = e / jnp.sum(e, axis=0, keepdims=True)
    high, low = split_two(probs)
    src = lax.broadcasted_iota(I32, (TOK, HELD), 0)
    dst = lax.broadcasted_iota(I32, (TOK, HELD), 1) % TOK
    copies = jnp.where(src == dst, 1.0, 0.0).astype(BF16)
    out[TOK:, :] = jnp.zeros((META, out.shape[1]), BF16)
    rows = jnp.concatenate(
        [routes[...].astype(F32), high.astype(F32), low.astype(F32), jnp.zeros((TOPK, TOK), F32)], axis=0
    )
    spread = dot(rows.astype(BF16), copies)
    out[TOK:, :HELD] = spread[:META].astype(BF16)
    out[TOK:, HELD : 2 * HELD] = spread[META:].astype(BF16)


def norm_block(tokens, gain, routes, logits):
    width = tokens.shape[1]
    return pl.pallas_call(
        norm_kernel,
        out_shape=jax.ShapeDtypeStruct((TOK + META, width), BF16),
        in_specs=[VMEM] * 4,
        out_specs=VMEM,
        name="norm",
        compiler_params=pltpu.CompilerParams(vmem_limit_bytes=4 * MIB),
    )(tokens, gain.reshape(1, width), routes, logits)


def build_kernel(where, b0, b1, b2, b3, own, out, aux, rows):
    first, mine = where[0], where[1] == 1
    blocks = (b0, b1, b2, b3)
    lane = lax.broadcasted_iota(I32, (META, HELD), 1) // TOK
    meta = [jnp.zeros((META, HELD), F32)] * 2
    for k, b in enumerate(blocks):
        for part in range(2):
            cols = slice(part * HELD, (part + 1) * HELD)
            piece = b[TOK:, cols].astype(F32)
            if k == 3:
                piece = jnp.where(mine, own[TOK:, cols].astype(F32), piece)
            meta[part] = jnp.where(lane == k, piece, meta[part])
        if k == 3:

            @pl.when(mine)
            def _():
                rows[k * TOK :, :] = own[:TOK, :]

            @pl.when(jnp.logical_not(mine))
            def _():
                rows[k * TOK :, :] = b[:TOK, :]
        else:
            rows[k * TOK : (k + 1) * TOK, :] = b[:TOK, :]
    ids = meta[0][:TOPK].astype(I32)
    prob = meta[0][TOPK:] + meta[1][:TOPK]
    expert = first + lax.broadcasted_iota(I32, (PLANE, HELD), 0)
    chosen = jnp.zeros((PLANE, HELD), F32)
    share = jnp.zeros((PLANE, HELD), F32)
    for j in range(TOPK):
        hit = ids[j : j + 1, :] == expert
        chosen = jnp.where(hit, 1.0, chosen)
        share = jnp.where(hit, prob[j : j + 1, :], share)
    earlier = lax.broadcasted_iota(I32, (HELD, HELD), 0)
    later = lax.broadcasted_iota(I32, (HELD, HELD), 1)
    before = (earlier < later) & (earlier // TOK == later // TOK)
    rank = dot(chosen.astype(BF16), jnp.where(before, 1.0, 0.0).astype(BF16))
    block = lax.broadcasted_iota(I32, (PLANE, HELD), 1) // TOK
    place = jnp.where(chosen > 0.0, (block * CAP).astype(F32) + rank, -1.0)
    aux[:PLANE, :] = place
    aux[PLANE:, :] = share
    held = rows[...]
    slot = lax.broadcasted_iota(I32, (SLOTS, HELD), 0).astype(F32)
    for q in range(0, PLANE, 4):
        pick = jnp.concatenate(
            [jnp.where(place[i : i + 1, :] == slot, 1.0, 0.0).astype(BF16) for i in range(q, q + 4)], axis=0
        )
        out[q * SLOTS : (q + 4) * SLOTS, :] = dot(pick, held).astype(BF16)


def build(where, got, own):
    width = own.shape[1]
    return pl.pallas_call(
        build_kernel,
        out_shape=(jax.ShapeDtypeStruct((ROWS, width), BF16), jax.ShapeDtypeStruct((2 * PLANE, HELD), F32)),
        in_specs=[SMEM] + [VMEM] * 5,
        out_specs=(VMEM, VMEM),
        scratch_shapes=[pltpu.VMEM((HELD, width), BF16)],
        name="build",
        compiler_params=pltpu.CompilerParams(vmem_limit_bytes=8 * MIB),
    )(where, *got, own)


def expert_kernel(where, x, g0, u0, d0, g1, u1, d1, out, hidden):
    core = where[0]
    half = g0.shape[1]
    tile = 256
    mine = pl.multiple_of(core * half, half)
    theirs = pl.multiple_of((1 - core) * half, half)

    @pl.loop(0, x.shape[0] // tile)
    def _(i):
        rows = pl.ds(pl.multiple_of(i * tile, tile), tile)
        part = x[rows, :]
        for gate, up, at in ((g0, u0, mine), (g1, u1, theirs)):
            g = jnp.minimum(dot(part, gate[...]), 7.0)
            l = jnp.clip(dot(part, up[...]), -7.0, 7.0)
            hidden[:, pl.ds(at, half)] = (g * jax.nn.sigmoid(1.702 * g) * (l + 1.0)).astype(BF16)
        for down, at in ((d0, mine), (d1, theirs)):
            out[rows, pl.ds(at, half)] = dot(hidden[...], down[...]).astype(BF16)


def expert(where, x, mine, theirs):
    n, width = x.shape
    return pl.pallas_call(
        expert_kernel,
        out_shape=jax.ShapeDtypeStruct((n, width), BF16),
        in_specs=[SMEM] + [VMEM] * 7,
        out_specs=VMEM,
        scratch_shapes=[pltpu.VMEM((256, width), BF16)],
        name="expert",
        compiler_params=pltpu.CompilerParams(vmem_limit_bytes=24 * MIB),
    )(where, x, *mine, *theirs)


def combine_kernel(back, aux, o0, o1, o2, o3):
    slot = lax.broadcasted_iota(I32, (SLOTS, HELD), 0).astype(F32)
    total = jnp.zeros((2 * HELD, back.shape[1]), F32)
    for q in range(0, PLANE, 4):
        parts = []
        for i in range(q, q + 4):
            w = jnp.where(aux[i : i + 1, :] == slot, aux[PLANE + i : PLANE + i + 1, :], 0.0)
            parts.append(jnp.concatenate(split_two(w), axis=1))
        weights = jnp.concatenate(parts, axis=0)
        total = total + dot(weights, back[q * SLOTS : (q + 4) * SLOTS, :], ((0,), (0,)))
    total = total[:HELD] + total[HELD:]
    for k, o in enumerate((o0, o1, o2, o3)):
        o[...] = total[k * TOK : (k + 1) * TOK].astype(BF16)


def combine(back, aux):
    width = back.shape[1]
    return pl.pallas_call(
        combine_kernel,
        out_shape=[jax.ShapeDtypeStruct((TOK, width), BF16)] * BLOCKS,
        in_specs=[VMEM] * 2,
        out_specs=[VMEM] * BLOCKS,
        name="combine",
        compiler_params=pltpu.CompilerParams(vmem_limit_bytes=8 * MIB),
    )(back, aux)


def total_kernel(where, r0, r1, r2, r3, own, keep, give):
    core, mine = where[0], where[1] == 1
    half = keep.shape[1]
    last = jnp.where(mine, own[...].astype(F32), r3[...].astype(F32))
    total = r0[...].astype(F32) + r1[...].astype(F32) + r2[...].astype(F32) + last
    low, high = total[:, :half], total[:, half:]
    keep[...] = jnp.where(core == 0, low, high)
    give[...] = jnp.where(core == 0, high, low)


def total_of(where, got, own):
    width = own.shape[1]
    return pl.pallas_call(
        total_kernel,
        out_shape=[jax.ShapeDtypeStruct((TOK, width // 2), F32)] * 2,
        in_specs=[SMEM] + [VMEM] * 5,
        out_specs=[VMEM] * 2,
        name="total",
        compiler_params=pltpu.CompilerParams(vmem_limit_bytes=4 * MIB),
    )(where, *got, own)


def spread_pairs():
    sets = []
    for same, other in ((4, 3), (2, 1), (-2, -1), (None, -3)):
        pairs = []
        for z in range(NZ):
            p = z % 2
            if same is not None:
                pairs.append((z * 2 + p, ((z + same) % NZ) * 2 + p))
            pairs.append((z * 2 + 1 - p, ((z + other) % NZ) * 2 + p))
        sets.append(pairs)
    return sets


def shards(tokens, norm_gain, routing, route_logits, w_gate, w_up, w_down):
    core = lax.axis_index("tp").astype(I32)
    z = lax.axis_index("z").astype(I32)
    width = tokens.shape[1]
    swap = [(0, 1), (1, 0)]
    own = (z % 2 == core).astype(I32)
    plane_own = jnp.stack([z * PLANE, own])
    core_own = jnp.stack([core, own])

    mine = (w_gate[0], w_up[0], w_down[0])
    theirs = [lax.ppermute(w, "tp", swap) for w in mine]

    block = norm_block(tokens, norm_gain, routing.T, route_logits.T)
    pairs = spread_pairs()
    got = [lax.ppermute(block, ("z", "tp"), p) for p in pairs]
    outbound, aux = build(plane_own, got, block)

    def across(x):
        x = x.reshape(PLANE, SLOTS, width)
        return lax.all_to_all(x, ("y", "x"), split_axis=0, concat_axis=0, tiled=True).reshape(ROWS, width)

    out = expert(core_own, across(outbound), mine, theirs)
    partial = combine(across(out), aux)
    returned = [lax.ppermute(partial[k], ("z", "tp"), [(b, a) for a, b in p]) for k, p in enumerate(pairs)]
    keep, give = total_of(core_own, returned, partial[3])
    return (keep + lax.ppermute(give, "tp", swap)).astype(BF16)


def solution(mesh):
    torus = Mesh(mesh.devices.reshape(NZ, NY, NX, 2), ("z", "y", "x", "tp"))
    ep = ("z", "y", "x")
    return jax.shard_map(
        shards,
        mesh=torus,
        in_specs=(
            P(ep, None),
            P(),
            P(ep, None),
            P(ep, None),
            P(ep, None, "tp"),
            P(ep, None, "tp"),
            P(ep, None, "tp"),
        ),
        out_specs=P(ep, "tp"),
        check_vma=False,
    )
```
